1024 devices in a mesh: ep: 64 (over z, core), tp: 16 (over y, x).
Axes of the slice: x: 4, y: 4, z: 32, core: 2. Of those that a mesh axis runs over, the one named last changes fastest.
Arguments:
- tokens: bfloat16 [8192, 2048], P('ep', 'tp')
- norm_gain: float32 [2048], P('tp'), may hold values from 0.1 to 1.9
- routing: int32 [8192, 2], P('ep'), may hold values from 0 to 31, all different within a row; in each aligned block of 128 rows (0 to 127, 128 to 255, ...) at most 10 rows name the same one
- route_weight: float32 [8192, 2], P('ep'), may hold values from 0.1 to 1
- gate_weight: bfloat16 [64, 2048, 3584], P('ep', None, 'tp'), may hold values from -0.125 to 0.125
- up_weight: bfloat16 [64, 2048, 3584], P('ep', None, 'tp'), may hold values from -0.125 to 0.125
- down_weight: bfloat16 [64, 3584, 2048], P('ep', None, 'tp')
- final_gain: float32 [2048], P('tp'), may hold values from 0.1 to 1.9
Outputs:
- mixed: bfloat16 [8192, 2048], P('ep', 'tp')
The draws below stay inside these ranges and needn't reach their ends.
Inputs may be any that keep to these rules, and one draw needn't show every extreme that they name: `routing`: each row names 2 different experts. Among the 128 rows of one device along ep (aligned blocks), no expert is named more than 10 times, a bound that some blocks reach.
All inputs are finite; a program needn't handle non-finite values.
Results may differ from the reference program's by a relative error of at most 0.0077.
Values may be sent and summed in bfloat16 or wider, within the bound.
No kernel may reach another device: no remote copies, remote signals or barrier semaphores. Data moves between devices by JAX's collectives and lax.ppermute only.
A program may use at most 32 MiB of HBM per device.

```python
import math
import jax
import jax.numpy as jnp
import numpy as np
from jax import lax

D = 2048
FF = 7168
TOPK = 2
TOK_DEV = 128
EXPERTS = 32
CAP = 10
TOKENS = 8192
N_EP = 64


def draw_tokens(key, part):
    column = jnp.arange(D, dtype=jnp.float32) / D
    values = jax.random.normal(key, (TOKENS, D), jnp.float32) * 10.0 ** (0.8 * column)
    return values.astype(jnp.bfloat16)


def draw_down_weight(key, part):
    column = jnp.arange(D, dtype=jnp.float32) / D
    scale = (FF // 2) ** (-0.5) * 10.0 ** (0.8 * column)
    values = jax.random.normal(key, (2 * EXPERTS, FF // 2, D), jnp.float32)
    return (values * scale).astype(jnp.bfloat16)


def block_scale(rng, dims, cuts, low, high):
    level, own = 1.0, jax.random.fold_in(rng, 6)
    for position, shards_of in cuts:
        steps = jnp.exp(jax.random.uniform(jax.random.fold_in(own, position), (shards_of,), jnp.float32, low / len(cuts), high / len(cuts)))
        level = level * jnp.repeat(steps, dims[position] // shards_of).reshape([-1 if axis == position else 1 for axis in range(len(dims))])
    return level


def shared_out(own_key, own, number, rows, count, top, most, lean):
    order = jax.random.permutation(own_key, count)
    crowded, usual = portions_of(count, rows * top, most, lean, True), portions_of(count, rows * top, most, lean, False)
    places = jnp.arange(count)

    def named(sizes, rotation):
        used = int((sizes > 0).sum())
        fixed = max(1, used // 4)
        passed = fixed + (places - fixed + rotation * (used - fixed)) % max(1, count - fixed)
        return jnp.zeros((count,), jnp.int32).at[order[jnp.where(places < fixed, places, passed)]].set(jnp.asarray(sizes, jnp.int32))

    sizes = jnp.where(number % 4 == 0, named(crowded, number // 4), named(usual, number - number // 4 - 1))
    mixed = jax.random.permutation(jax.random.fold_in(own, 3), count)
    source_of, receiver = mixed[0:count // 2 * 2:2], mixed[1:count // 2 * 2:2]
    room = jnp.minimum(sizes[source_of] - 1, most - sizes[receiver]) // 2
    room = jnp.where((source_of == order[0]) | (receiver == order[0]) | (sizes[receiver] == 0), 0, jnp.maximum(room, 0))
    passed = jax.random.randint(jax.random.fold_in(own, 4), (count // 2,), 0, 1 << 20) % (room + 1)
    sizes = sizes.at[source_of].add(-passed).at[receiver].add(passed)
    members = jnp.searchsorted(jnp.cumsum(sizes), jnp.arange(rows * top), side="right").astype(jnp.int32)
    grid = members.reshape(top, rows).T
    grid = grid[jax.random.permutation(jax.random.fold_in(own, 1), rows)]
    rotation = jax.random.randint(jax.random.fold_in(own, 2), (rows, 1), 0, top)
    return jnp.take_along_axis(grid, (jnp.arange(top)[None, :] + rotation) % top, axis=1)


def portions_of(amount, total, limit, lean, full):
    portions = [(1 << 20) // math.isqrt(standing ** lean) + 1 for standing in range(1, amount + 1)]
    largest = limit if full else min(limit, max(-(-total // amount), total * portions[0] // sum(portions)))
    least = 1 if total - largest >= amount - 1 else 0
    given, surplus = [largest] + [least] * (amount - 1), total - largest - least * (amount - 1)
    while surplus > 0:
        movable = [i for i in range(1, amount) if given[i] < largest] or [i for i in range(1, amount) if given[i] < limit]
        pool, budget = sum([portions[i] for i in movable]), surplus
        for i in movable:
            extra = min(limit - given[i], max(1, budget * portions[i] // pool), surplus)
            given[i] = given[i] + extra
            surplus = surplus - extra
    return np.array(given)


def scatter_about(key, extent, deviation, most, shards=(), held_as=jnp.bfloat16):
    array = jax.random.normal(key, extent, jnp.float32) * deviation
    if len(shards) > 0:
        array = block_scale(key, extent, shards, -0.22, 0.18) * array
    return jnp.clip(array, min=-most, max=most).astype(held_as)


def setup_inputs(seed: int = 0) -> dict:
    seeds = jax.random.split(jax.random.key(seed), 9)
    tokens = draw_tokens(jax.random.fold_in(seeds[8], 71), 0)
    norm_gain = jnp.clip(1.0 + 0.18 * jax.random.normal(seeds[1], (D,), jnp.float32), 0.1, 1.9)
    routing_keys = jax.random.split(jax.random.fold_in(seeds[2], 1), TOKENS // TOK_DEV)
    routing_turns = jax.random.permutation(jax.random.fold_in(seeds[2], 3), TOKENS // TOK_DEV)
    routing = jax.vmap(lambda own, number: shared_out(jax.random.fold_in(seeds[2], 2), own, number, TOK_DEV, EXPERTS, TOPK, CAP, 2))(routing_keys, routing_turns).reshape((TOKENS, TOPK))
    route_weight = jnp.clip(0.1 + 0.9 * jax.random.uniform(seeds[3], (TOKENS, TOPK), jnp.float32) ** block_scale(seeds[3], (TOKENS, TOPK), ((0, 64),), -0.2, 0.2), 0.1, 1.0)
    gate_weight = scatter_about(seeds[4], (2 * EXPERTS, D, FF // 2), D ** -0.5, 0.125, ((0, 64), (2, 16)))
    up_weight = scatter_about(seeds[5], (2 * EXPERTS, D, FF // 2), D ** -0.5, 0.125, ((0, 64), (2, 16)))
    down_weight = draw_down_weight(jax.random.fold_in(seeds[8], 71), 0)
    final_gain = jnp.clip(1.0 + 0.18 * jax.random.normal(seeds[7], (D,), jnp.float32), 0.1, 1.9)
    return dict(tokens=tokens, norm_gain=norm_gain, routing=routing, route_weight=route_weight, gate_weight=gate_weight, up_weight=up_weight, down_weight=down_weight, final_gain=final_gain)


EPS = 1e-05

def rms_scale(values, gain):
    return values * lax.rsqrt(lax.optimization_barrier(jnp.mean(values * values, axis=-1, keepdims=True)) + EPS) * gain

def slot_numbers(expert_ids):
    onehot = (expert_ids[..., None] == jnp.arange(EXPERTS, dtype=jnp.int32)).astype(jnp.int32)
    before = jnp.cumsum(onehot, axis=1) - onehot
    return lax.optimization_barrier(jnp.sum(before * onehot, axis=2)).astype(jnp.int32)

def reference(tokens, norm_gain, routing, route_weight, gate_weight, up_weight, down_weight, final_gain):
    normed = rms_scale(tokens.astype(jnp.float32), norm_gain).astype(jnp.bfloat16)
    copies = TOK_DEV * TOPK
    expert_ids = routing.reshape(N_EP, copies).astype(jnp.int32)
    slot_index = slot_numbers(expert_ids)
    source_index = jnp.broadcast_to(jnp.arange(N_EP, dtype=jnp.int32)[:, None], (N_EP, copies))
    token_index = jnp.broadcast_to((jnp.arange(copies, dtype=jnp.int32) // TOPK)[None, :], (N_EP, copies))
    source_rows = normed.reshape(N_EP, TOK_DEV, D)[source_index, token_index]

    def one_expert(expert):
        target = jnp.where(expert_ids == expert, slot_index, CAP)
        buffer = jnp.zeros((N_EP, CAP, D), jnp.bfloat16).at[source_index, target].set(source_rows, mode='drop')
        buffer = buffer.reshape(N_EP * CAP, D)
        results = []
        for half_index in range(2):
            row = 2 * expert + half_index
            gate_half = lax.dynamic_index_in_dim(gate_weight, row, 0, keepdims=False)
            up_half = lax.dynamic_index_in_dim(up_weight, row, 0, keepdims=False)
            down_half = lax.dynamic_index_in_dim(down_weight, row, 0, keepdims=False)
            gate = jnp.dot(buffer, gate_half, preferred_element_type=jnp.float32)
            upper = jnp.dot(buffer, up_half, preferred_element_type=jnp.float32)
            hidden = (jax.nn.silu(gate) * upper).astype(jnp.bfloat16)
            results.append(jnp.dot(hidden, down_half, preferred_element_type=jnp.float32).astype(jnp.bfloat16))
        return jnp.stack(results)
    results = lax.map(one_expert, jnp.arange(EXPERTS, dtype=jnp.int32))
    results = results.reshape(EXPERTS, 2, N_EP, CAP, D)
    picked = results[expert_ids, :, source_index, slot_index]
    paired = (picked[:, :, 0].astype(jnp.float32) + picked[:, :, 1].astype(jnp.float32)).astype(jnp.bfloat16)
    paired = lax.optimization_barrier(paired)
    summed = paired.astype(jnp.float32)
    weights = route_weight.reshape(N_EP, copies).astype(jnp.float32)
    mixed_sum = lax.optimization_barrier(jnp.sum((summed * weights[..., None]).reshape(N_EP, TOK_DEV, TOPK, D), axis=2))
    mixed_sum = mixed_sum.reshape(TOKENS, D)
    return rms_scale(mixed_sum, final_gain).astype(jnp.bfloat16)
```

```python
import jax
import jax.numpy as jnp
from jax import lax
from jax.experimental import pallas as pl
from jax.experimental.pallas import tpu as pltpu
from jax.sharding import Mesh, PartitionSpec as P

D = 2048
EXPERTS = 32
TOK = 128
CAP = 10
ROWS = EXPERTS * CAP
TP = 16
W = D // TP
HID = 224
EXTRA = 8
EPS = 1e-05

VMEM = pl.BlockSpec(memory_space=pltpu.VMEM)
F32 = jnp.float32
BF16 = jnp.bfloat16


def call(kernel, out_shape, count, **kw):
    many = isinstance(out_shape, (tuple, list))
    return pl.pallas_call(
        kernel,
        out_shape=out_shape,
        in_specs=[VMEM] * count,
        out_specs=tuple(VMEM for _ in out_shape) if many else VMEM,
        **kw,
    )


def place_of(slot, expert):
    return (slot // 2) * (2 * EXPERTS) + 2 * expert + slot % 2


def dispatch_kernel(routing_ref, tokens_ref, gain_ref, out_ref, place_ref, gain_out_ref):
    routing = routing_ref[...]
    expert0, expert1 = routing[:, 0:1], routing[:, 1:2]
    lanes = lax.broadcasted_iota(jnp.int32, (TOK, 128), 1)
    hit0, hit1 = lanes == expert0, lanes == expert1
    both = jnp.where(hit0 | hit1, 1.0, 0.0).astype(BF16)
    earlier = jnp.where(
        lax.broadcasted_iota(jnp.int32, (TOK, TOK), 1)
        < lax.broadcasted_iota(jnp.int32, (TOK, TOK), 0),
        1.0,
        0.0,
    ).astype(BF16)
    before = jnp.dot(earlier, both, preferred_element_type=F32)
    slot0 = jnp.sum(jnp.where(hit0, before, 0.0), axis=1, keepdims=True).astype(jnp.int32)
    slot1 = jnp.sum(jnp.where(hit1, before, 0.0), axis=1, keepdims=True).astype(jnp.int32)
    place0, place1 = place_of(slot0, expert0), place_of(slot1, expert1)
    place_ref[...] = jnp.concatenate([place0, place1], axis=1)
    spots = lax.broadcasted_iota(jnp.int32, (TOK, ROWS), 1)
    picker = jnp.where((spots == place0) | (spots == place1), 1.0, 0.0).astype(BF16)
    rows = lax.dot_general(
        picker, tokens_ref[...], (((0,), (0,)), ((), ())), preferred_element_type=F32
    ).astype(BF16)
    for block in range(CAP // 2):
        out_ref[:, block * W : (block + 1) * W] = rows[block * 64 : (block + 1) * 64]
    gain = gain_ref[...]
    high = gain.astype(BF16).astype(F32)
    mid = (gain - high).astype(BF16).astype(F32)
    low = gain - high - mid
    index = lax.broadcasted_iota(jnp.int32, (EXTRA, W), 0)
    parts = jnp.where(index == 0, high, jnp.where(index == 1, mid, jnp.where(index == 2, low, 0.0)))
    gain_out_ref[...] = parts.astype(BF16)


def spread_kernel(rows_ref, gain_ref, out_ref):
    gain = gain_ref[...]
    for block in range(CAP // 2):
        piece = rows_ref[:, block * W : (block + 1) * W]
        for peer in range(TP):
            out_ref[peer, block * 64 : (block + 1) * 64] = piece
    for peer in range(TP):
        out_ref[peer, ROWS : ROWS + EXTRA] = gain


def experts_kernel(x_ref, gate_a, gate_b, up_a, up_b, down_a, down_b, out_ref, normed_ref):
    total = jnp.zeros((ROWS, W), F32)
    for t in range(TP):
        piece = x_ref[t, :ROWS].astype(F32)
        total = total + piece * piece
    scale = lax.rsqrt(jnp.sum(total, axis=1, keepdims=True) / D + EPS)
    for t in range(TP):
        gain = jnp.sum(x_ref[t, ROWS : ROWS + EXTRA].astype(F32), axis=0, keepdims=True)
        piece = x_ref[t, :ROWS].astype(F32)
        normed_ref[:, t * W : (t + 1) * W] = (piece * scale * gain).astype(BF16)
    normed = normed_ref[...]
    hidden = []
    for gate_ref, up_ref in ((gate_a, up_a), (gate_b, up_b)):
        gate = jnp.dot(normed, gate_ref[...], preferred_element_type=F32)
        upper = jnp.dot(normed, up_ref[...], preferred_element_type=F32)
        hidden.append((jax.nn.silu(gate) * upper).astype(BF16))
    for t in range(TP):
        part = jnp.dot(hidden[0], down_a[t], preferred_element_type=F32)
        part = part + jnp.dot(hidden[1], down_b[t], preferred_element_type=F32)
        out_ref[t] = part.astype(BF16)


def reduce_kernel(parts_ref, out_ref):
    for block in range(CAP // 2):
        total = jnp.zeros((64, W), F32)
        for t in range(TP):
            total = total + parts_ref[t, block * 64 : (block + 1) * 64].astype(F32)
        out_ref[:, block * W : (block + 1) * W] = total.astype(BF16)


def combine_kernel(rows_ref, place_ref, weight_ref, mixed_ref, square_ref):
    rows = jnp.concatenate(
        [rows_ref[:, block * W : (block + 1) * W] for block in range(CAP // 2)], axis=0
    )
    spots = lax.broadcasted_iota(jnp.int32, (TOK, ROWS), 1)
    mixed = jnp.zeros((TOK, W), F32)
    for k in range(2):
        pick = jnp.where(spots == place_ref[:, k : k + 1], 1.0, 0.0).astype(BF16)
        row = jnp.dot(pick, rows, preferred_element_type=F32)
        mixed = mixed + row * weight_ref[:, k : k + 1]
    mixed_ref[...] = mixed
    square = jnp.sum((mixed * mixed).T, axis=0, keepdims=True)
    for t in range(TP):
        square_ref[t] = square


def finish_kernel(mixed_ref, square_ref, gain_ref, out_ref):
    square = jnp.zeros((1, TOK), F32)
    for t in range(TP):
        square = square + square_ref[t]
    column = jnp.broadcast_to(lax.rsqrt(square / D + EPS), (TOK, TOK)).T
    out_ref[...] = (mixed_ref[...] * column * gain_ref[...]).astype(BF16)


def shards(
    tokens, norm_gain, routing, route_weight, gate_weight, up_weight, down_weight, final_gain
):
    swap = [(0, 1), (1, 0)]
    gate_own, up_own = gate_weight[0], up_weight[0]
    outgoing, place, gain_parts = call(
        dispatch_kernel,
        (
            jax.ShapeDtypeStruct((64, 640), BF16),
            jax.ShapeDtypeStruct((TOK, 2), jnp.int32),
            jax.ShapeDtypeStruct((EXTRA, W), BF16),
        ),
        3,
    )(routing, tokens, norm_gain.reshape(1, W))
    arrived = lax.all_to_all(
        outgoing.reshape(EXPERTS, 2, 640), "z", 0, 0, tiled=True
    ).reshape(64, 640)
    down_own = lax.all_to_all(
        down_weight.reshape(TP, HID, W), "t", 0, 0, tiled=True
    )
    gate_other = lax.ppermute(gate_own, "c", swap)
    up_other = lax.ppermute(up_own, "c", swap)
    down_other = lax.ppermute(down_own, "c", swap)
    spread = call(
        spread_kernel, jax.ShapeDtypeStruct((TP, ROWS + EXTRA, W), BF16), 2
    )(arrived, gain_parts)
    features = lax.all_to_all(spread, "t", 0, 0, tiled=True)
    parts = call(
        experts_kernel,
        jax.ShapeDtypeStruct((TP, ROWS, W), BF16),
        7,
        scratch_shapes=[pltpu.VMEM((ROWS, D), BF16)],
    )(features, gate_own, gate_other, up_own, up_other, down_own, down_other)
    parts = lax.all_to_all(parts, "t", 0, 0, tiled=True)
    reduced = call(reduce_kernel, jax.ShapeDtypeStruct((64, 640), BF16), 1)(parts)
    returned = lax.all_to_all(
        reduced.reshape(EXPERTS, 2, 640), "z", 0, 0, tiled=True
    ).reshape(64, 640)
    mixed, square = call(
        combine_kernel,
        (
            jax.ShapeDtypeStruct((TOK, W), F32),
            jax.ShapeDtypeStruct((TP, 1, TOK), F32),
        ),
        3,
    )(returned, place, route_weight)
    squares = lax.all_to_all(square, "t", 0, 0, tiled=True)
    return call(finish_kernel, jax.ShapeDtypeStruct((TOK, W), BF16), 3)(
        mixed, squares, final_gain.reshape(1, W)
    )


def solution(mesh):
    split = Mesh(mesh.devices.reshape(EXPERTS, 2, TP), ("z", "c", "t"))
    ep = ("z", "c")
    placed = (
        P(ep, "t"),
        P("t"),
        P(ep, None),
        P(ep, None),
        P(ep, None, "t"),
        P(ep, None, "t"),
        P(ep, None, "t"),
        P("t"),
    )
    return jax.shard_map(
        shards, mesh=split, in_specs=placed, out_specs=P(ep, "t"), check_vma=False
    )
```

```python
import jax
import jax.numpy as jnp
from jax import lax
from jax.experimental import pallas as pl
from jax.experimental.pallas import tpu as pltpu
from jax.sharding import Mesh, PartitionSpec as P


D = 2048
EXPERTS = 32
TOK = 128
CAP = 10
ROWS = EXPERTS * CAP
TP = 16
W = D // TP
HID = 224
EXTRA = 8
EPS = 1e-05

F32 = jnp.float32
BF16 = jnp.bfloat16
MIB = 1 << 20


def call(kernel, outs, mib, free=0, **kw):
    def run(*operands):
        near = operands[: len(operands) - free]
        far = operands[len(operands) - free :]
        many = isinstance(outs, list)
        vmem = pl.BlockSpec(memory_space=pltpu.VMEM)
        return pl.pallas_call(
            kernel,
            out_shape=[pltpu.VMEM(s, d) for s, d in outs] if many else pltpu.VMEM(*outs),
            in_specs=[vmem] * len(near) + [pl.BlockSpec(memory_space=pl.ANY)] * free,
            out_specs=[vmem] * len(outs) if many else vmem,
            compiler_params=pltpu.CompilerParams(vmem_limit_bytes=mib * MIB),
            **kw,
        )(*[pltpu.with_memory_space_constraint(x, pltpu.VMEM) for x in near], *far)

    return run


def place_of(slot, expert):
    return (slot // 2) * (2 * EXPERTS) + 2 * expert + slot % 2


def dispatch_kernel(routing_ref, tokens_ref, gain_ref, out_ref, place_ref, gain_out_ref):
    expert0, expert1 = routing_ref[0:1], routing_ref[1:2]
    index = lax.broadcasted_iota(jnp.int32, (EXPERTS, TOK), 0)
    hit0, hit1 = index == expert0, index == expert1
    both = jnp.where(hit0 | hit1, 1.0, 0.0).astype(BF16)
    earlier = jnp.where(
        lax.broadcasted_iota(jnp.int32, (TOK, TOK), 0)
        < lax.broadcasted_iota(jnp.int32, (TOK, TOK), 1),
        1.0,
        0.0,
    ).astype(BF16)
    before = jnp.dot(both, earlier, preferred_element_type=F32)
    slot0 = jnp.sum(jnp.where(hit0, before, 0.0), axis=0, keepdims=True).astype(jnp.int32)
    slot1 = jnp.sum(jnp.where(hit1, before, 0.0), axis=0, keepdims=True).astype(jnp.int32)
    place0, place1 = place_of(slot0, expert0), place_of(slot1, expert1)
    place_ref[0:1] = place0
    place_ref[1:2] = place1
    spots = lax.broadcasted_iota(jnp.int32, (ROWS, TOK), 0)
    picker = jnp.where((spots == place0) | (spots == place1), 1.0, 0.0).astype(BF16)
    rows = jnp.dot(picker, tokens_ref[...], preferred_element_type=F32).astype(BF16)
    for block in range(CAP // 2):
        piece = rows[block * 64 : (block + 1) * 64]
        out_ref[:, :, block * W : (block + 1) * W] = piece.reshape(EXPERTS, 2, W)
    gain = gain_ref[...]
    high = gain.astype(BF16).astype(F32)
    mid = (gain - high).astype(BF16).astype(F32)
    low = gain - high - mid
    part = lax.broadcasted_iota(jnp.int32, (EXTRA, W), 0)
    parts = jnp.where(part == 0, high, jnp.where(part == 1, mid, jnp.where(part == 2, low, 0.0)))
    gain_out_ref[...] = parts.astype(BF16)


def prepare_kernel(place_ref, weight_ref, pick_ref, weight_out_ref):
    spots = lax.broadcasted_iota(jnp.int32, (TOK, ROWS), 1).astype(F32)
    for k in range(2):
        place = jnp.broadcast_to(place_ref[k : k + 1].astype(F32), (TOK, TOK)).T
        pick_ref[k] = jnp.where(spots == place[:, 0:1], 1.0, 0.0).astype(BF16)
        weight_out_ref[k] = jnp.broadcast_to(weight_ref[k : k + 1], (TOK, TOK)).T


def spread_kernel(rows_ref, gain_ref, out_ref):
    gain = gain_ref[...]
    for block in range(CAP // 2):
        piece = rows_ref[:, :, block * W : (block + 1) * W].reshape(64, W)
        for peer in range(TP):
            out_ref[peer, block * 64 : (block + 1) * 64] = piece
    for peer in range(TP):
        out_ref[peer, ROWS : ROWS + EXTRA] = gain


def experts_kernel(x_ref, gate_a, gate_b, up_a, up_b, down_a, down_b, out_ref, normed_ref):
    total = jnp.zeros((ROWS, W), F32)
    for t in range(TP):
        piece = x_ref[t, :ROWS].astype(F32)
        total = total + piece * piece
    scale = lax.rsqrt(jnp.sum(total, axis=1, keepdims=True) / D + EPS)
    for t in range(TP):
        gain = jnp.sum(x_ref[t, ROWS : ROWS + EXTRA].astype(F32), axis=0, keepdims=True)
        piece = x_ref[t, :ROWS].astype(F32)
        normed_ref[:, t * W : (t + 1) * W] = (piece * scale * gain).astype(BF16)
    normed = normed_ref[...]
    hidden = []
    across = (((1,), (1,)), ((), ()))
    for gate_ref, up_ref in ((gate_a, up_a), (gate_b, up_b)):
        gate = lax.dot_general(normed, gate_ref[...], across, preferred_element_type=F32)
        upper = lax.dot_general(normed, up_ref[...], across, preferred_element_type=F32)
        hidden.append((jax.nn.silu(gate) * upper).astype(BF16))
    for t in range(TP):
        part = jnp.dot(hidden[0], down_a[t], preferred_element_type=F32)
        part = part + jnp.dot(hidden[1], down_b[t], preferred_element_type=F32)
        out_ref[t] = part.astype(BF16)


def reduce_kernel(parts_ref, out_ref):
    for block in range(CAP // 2):
        total = jnp.zeros((64, W), F32)
        for t in range(TP):
            total = total + parts_ref[t, block * 64 : (block + 1) * 64].astype(F32)
        out_ref[:, :, block * W : (block + 1) * W] = total.astype(BF16).reshape(EXPERTS, 2, W)


def combine_kernel(rows_ref, pick_ref, weight_ref, mixed_ref, square_ref):
    rows = jnp.concatenate(
        [
            rows_ref[:, :, block * W : (block + 1) * W].reshape(64, W)
            for block in range(CAP // 2)
        ],
        axis=0,
    )
    mixed = jnp.zeros((TOK, W), F32)
    for k in range(2):
        row = jnp.dot(pick_ref[k], rows, preferred_element_type=F32)
        mixed = mixed + row * weight_ref[k]
    mixed_ref[...] = mixed
    square = jnp.sum((mixed * mixed).T, axis=0, keepdims=True)
    for t in range(TP):
        square_ref[t] = square


def finish_kernel(mixed_ref, square_ref, gain_ref, out_ref):
    square = jnp.zeros((1, TOK), F32)
    for t in range(TP):
        square = square + square_ref[t]
    column = jnp.broadcast_to(lax.rsqrt(square / D + EPS), (TOK, TOK)).T
    out_ref[...] = (mixed_ref[...] * column * gain_ref[...]).astype(BF16)


def shards(
    tokens, norm_gain, routing, route_weight, gate_weight, up_weight, down_weight, final_gain
):
    swap = [(0, 1), (1, 0)]
    gate_own, up_own = gate_weight[0].T, up_weight[0].T
    outgoing, place, gain_parts = call(
        dispatch_kernel,
        [((EXPERTS, 2, 640), BF16), ((2, TOK), jnp.int32), ((EXTRA, W), BF16)],
        4,
    )(routing.T, tokens, norm_gain.reshape(1, W))
    arrived = lax.all_to_all(outgoing, "z", 0, 0, tiled=True)
    down_own = lax.all_to_all(down_weight.reshape(TP, HID, W), "t", 0, 0, tiled=True)
    gate_other = lax.ppermute(gate_own, "c", swap)
    up_other = lax.ppermute(up_own, "c", swap)
    down_other = lax.ppermute(down_own, "c", swap)
    pick, weight = call(
        prepare_kernel,
        [((2, TOK, ROWS), BF16), ((2, TOK, W), F32)],
        4,
    )(place, route_weight.T)
    spread = call(spread_kernel, ((TP, ROWS + EXTRA, W), BF16), 4)(arrived, gain_parts)
    features = lax.all_to_all(spread, "t", 0, 0, tiled=True)
    parts = call(
        experts_kernel,
        ((TP, ROWS, W), BF16),
        24,
        scratch_shapes=[pltpu.VMEM((ROWS, D), BF16)],
    )(features, gate_own, gate_other, up_own, up_other, down_own, down_other)
    parts = lax.all_to_all(parts, "t", 0, 0, tiled=True)
    reduced = call(reduce_kernel, ((EXPERTS, 2, 640), BF16), 4)(parts)
    returned = lax.all_to_all(reduced, "z", 0, 0, tiled=True)
    mixed, square = call(
        combine_kernel, [((TOK, W), F32), ((TP, 1, TOK), F32)], 4
    )(returned, pick, weight)
    squares = lax.all_to_all(square, "t", 0, 0, tiled=True)
    return call(finish_kernel, ((TOK, W), BF16), 4)(mixed, squares, final_gain.reshape(1, W))


def solution(mesh):
    split = Mesh(mesh.devices.reshape(EXPERTS, 2, TP), ("z", "c", "t"))
    ep = ("z", "c")
    placed = (
        P(ep, "t"),
        P("t"),
        P(ep, None),
        P(ep, None),
        P(ep, None, "t"),
        P(ep, None, "t"),
        P(ep, None, "t"),
        P("t"),
    )
    return jax.shard_map(
        shards, mesh=split, in_specs=placed, out_specs=P(ep, "t"), check_vma=False
    )
```

```python
import jax
import jax.numpy as jnp
from jax import lax
from jax.experimental import pallas as pl
from jax.experimental.pallas import tpu as pltpu
from jax.sharding import Mesh, PartitionSpec as P


D = 2048
EXPERTS = 32
TOK = 128
CAP = 10
ROWS = EXPERTS * CAP
TP = 16
W = D // TP
HID = 224
EXTRA = 8
FRONT = ROWS + EXTRA
EPS = 1e-05

F32 = jnp.float32
BF16 = jnp.bfloat16
MIB = 1 << 20


def call(kernel, outs, mib, free=0, **kw):
    def run(*operands):
        near = operands[: len(operands) - free]
        far = operands[len(operands) - free :]
        many = isinstance(outs, list)
        vmem = pl.BlockSpec(memory_space=pltpu.VMEM)
        return pl.pallas_call(
            kernel,
            out_shape=[pltpu.VMEM(s, d) for s, d in outs] if many else pltpu.VMEM(*outs),
            in_specs=[vmem] * len(near) + [pl.BlockSpec(memory_space=pl.ANY)] * free,
            out_specs=[vmem] * len(outs) if many else vmem,
            compiler_params=pltpu.CompilerParams(vmem_limit_bytes=mib * MIB),
            **kw,
        )(*[pltpu.with_memory_space_constraint(x, pltpu.VMEM) for x in near], *far)

    return run


def place_of(slot, expert):
    return (slot // 2) * (2 * EXPERTS) + 2 * expert + slot % 2


def dispatch_kernel(routing_ref, tokens_ref, gain_ref, out_ref, place_ref, gain_out_ref):
    expert0, expert1 = routing_ref[0:1], routing_ref[1:2]
    index = lax.broadcasted_iota(jnp.int32, (EXPERTS, TOK), 0)
    hit0, hit1 = index == expert0, index == expert1
    both = jnp.where(hit0 | hit1, 1.0, 0.0).astype(BF16)
    earlier = jnp.where(
        lax.broadcasted_iota(jnp.int32, (TOK, TOK), 0)
        < lax.broadcasted_iota(jnp.int32, (TOK, TOK), 1),
        1.0,
        0.0,
    ).astype(BF16)
    before = jnp.dot(both, earlier, preferred_element_type=F32)
    slot0 = jnp.sum(jnp.where(hit0, before, 0.0), axis=0, keepdims=True).astype(jnp.int32)
    slot1 = jnp.sum(jnp.where(hit1, before, 0.0), axis=0, keepdims=True).astype(jnp.int32)
    place0, place1 = place_of(slot0, expert0), place_of(slot1, expert1)
    place_ref[0:1] = place0
    place_ref[1:2] = place1
    spots = lax.broadcasted_iota(jnp.int32, (ROWS, TOK), 0)
    picker = jnp.where((spots == place0) | (spots == place1), 1.0, 0.0).astype(BF16)
    rows = jnp.dot(picker, tokens_ref[...], preferred_element_type=F32).astype(BF16)
    for block in range(CAP // 2):
        piece = rows[block * 64 : (block + 1) * 64]
        out_ref[:, :, block * W : (block + 1) * W] = piece.reshape(EXPERTS, 2, W)
    gain = gain_ref[...]
    high = gain.astype(BF16).astype(F32)
    mid = (gain - high).astype(BF16).astype(F32)
    low = gain - high - mid
    part = lax.broadcasted_iota(jnp.int32, (EXTRA, W), 0)
    parts = jnp.where(part == 0, high, jnp.where(part == 1, mid, jnp.where(part == 2, low, 0.0)))
    gain_out_ref[...] = parts.astype(BF16)


def prepare_kernel(place_ref, weight_ref, gate_ref, up_ref, pick_ref, weight_out_ref):
    del gate_ref, up_ref
    spots = lax.broadcasted_iota(jnp.int32, (TOK, ROWS), 1).astype(F32)
    for k in range(2):
        place = jnp.broadcast_to(place_ref[k : k + 1].astype(F32), (TOK, TOK)).T
        pick_ref[k] = jnp.where(spots == place[:, 0:1], 1.0, 0.0).astype(BF16)
        weight_out_ref[k] = jnp.broadcast_to(weight_ref[k : k + 1], (TOK, TOK)).T


def spread_kernel(rows_ref, gain_ref, down_ref, out_ref):
    gain = gain_ref[...]
    for block in range(CAP // 2):
        piece = rows_ref[:, :, block * W : (block + 1) * W].reshape(64, W)
        for peer in range(TP):
            out_ref[peer, block * 64 : (block + 1) * 64] = piece
    for peer in range(TP):
        out_ref[peer, ROWS:FRONT] = gain
        out_ref[peer, FRONT:] = down_ref[peer]


def hidden_kernel(x_ref, gate_a, gate_b, up_a, up_b, out_ref, normed_ref):
    total = jnp.zeros((ROWS, W), F32)
    for t in range(TP):
        piece = x_ref[t, :ROWS].astype(F32)
        total = total + piece * piece
    scale = lax.rsqrt(jnp.sum(total, axis=1, keepdims=True) / D + EPS)
    for t in range(TP):
        gain = jnp.sum(x_ref[t, ROWS:FRONT].astype(F32), axis=0, keepdims=True)
        piece = x_ref[t, :ROWS].astype(F32)
        normed_ref[:, t * W : (t + 1) * W] = (piece * scale * gain).astype(BF16)
    normed = normed_ref[...]
    across = (((1,), (1,)), ((), ()))
    for half, (gate_ref, up_ref) in enumerate(((gate_a, up_a), (gate_b, up_b))):
        gate = lax.dot_general(normed, gate_ref[...], across, preferred_element_type=F32)
        upper = lax.dot_general(normed, up_ref[...], across, preferred_element_type=F32)
        out_ref[half] = (jax.nn.silu(gate) * upper).astype(BF16)


def output_kernel(hidden_ref, x_ref, down_ref, out_ref):
    first, second = hidden_ref[0], hidden_ref[1]
    for t in range(TP):
        part = jnp.dot(first, x_ref[t, FRONT:], preferred_element_type=F32)
        part = part + jnp.dot(second, down_ref[t], preferred_element_type=F32)
        out_ref[t] = part.astype(BF16)


def reduce_kernel(parts_ref, out_ref):
    for block in range(CAP // 2):
        total = jnp.zeros((64, W), F32)
        for t in range(TP):
            total = total + parts_ref[t, block * 64 : (block + 1) * 64].astype(F32)
        out_ref[:, :, block * W : (block + 1) * W] = total.astype(BF16).reshape(EXPERTS, 2, W)


def combine_kernel(rows_ref, pick_ref, weight_ref, mixed_ref, square_ref):
    rows = jnp.concatenate(
        [
            rows_ref[:, :, block * W : (block + 1) * W].reshape(64, W)
            for block in range(CAP // 2)
        ],
        axis=0,
    )
    mixed = jnp.zeros((TOK, W), F32)
    for k in range(2):
        row = jnp.dot(pick_ref[k], rows, preferred_element_type=F32)
        mixed = mixed + row * weight_ref[k]
    mixed_ref[...] = mixed
    square = jnp.sum((mixed * mixed).T, axis=0, keepdims=True)
    for t in range(TP):
        square_ref[t] = square


def finish_kernel(mixed_ref, square_ref, gain_ref, out_ref):
    square = jnp.zeros((1, TOK), F32)
    for t in range(TP):
        square = square + square_ref[t]
    column = jnp.broadcast_to(lax.rsqrt(square / D + EPS), (TOK, TOK)).T
    out_ref[...] = (mixed_ref[...] * column * gain_ref[...]).astype(BF16)


def shards(
    tokens, norm_gain, routing, route_weight, gate_weight, up_weight, down_weight, final_gain
):
    swap = [(0, 1), (1, 0)]
    gate_own, up_own = gate_weight[0].T, up_weight[0].T
    outgoing, place, gain_parts = call(
        dispatch_kernel,
        [((EXPERTS, 2, 640), BF16), ((2, TOK), jnp.int32), ((EXTRA, W), BF16)],
        4,
    )(routing.T, tokens, norm_gain.reshape(1, W))
    arrived = lax.all_to_all(outgoing, "z", 0, 0, tiled=True)
    gate_other = lax.ppermute(gate_own, "c", swap)
    up_other = lax.ppermute(up_own, "c", swap)
    pick, weight = call(
        prepare_kernel,
        [((2, TOK, ROWS), BF16), ((2, TOK, W), F32)],
        4,
        free=2,
    )(place, route_weight.T, gate_other, up_other)
    spread = call(spread_kernel, ((TP, FRONT + HID, W), BF16), 4)(
        arrived, gain_parts, down_weight.reshape(TP, HID, W)
    )
    features = lax.all_to_all(spread, "t", 0, 0, tiled=True)
    down_other = lax.ppermute(features[:, FRONT:], "c", swap)
    hidden = call(
        hidden_kernel,
        ((2, ROWS, HID), BF16),
        16,
        scratch_shapes=[pltpu.VMEM((ROWS, D), BF16)],
    )(features, gate_own, gate_other, up_own, up_other)
    parts = call(output_kernel, ((TP, ROWS, W), BF16), 8)(
        hidden, features, down_other
    )
    parts = lax.all_to_all(parts, "t", 0, 0, tiled=True)
    reduced = call(reduce_kernel, ((EXPERTS, 2, 640), BF16), 4)(parts)
    returned = lax.all_to_all(reduced, "z", 0, 0, tiled=True)
    mixed, square = call(
        combine_kernel, [((TOK, W), F32), ((TP, 1, TOK), F32)], 4
    )(returned, pick, weight)
    squares = lax.all_to_all(square, "t", 0, 0, tiled=True)
    return call(finish_kernel, ((TOK, W), BF16), 4)(mixed, squares, final_gain.reshape(1, W))


def solution(mesh):
    split = Mesh(mesh.devices.reshape(EXPERTS, 2, TP), ("z", "c", "t"))
    ep = ("z", "c")
    placed = (
        P(ep, "t"),
        P("t"),
        P(ep, None),
        P(ep, None),
        P(ep, None, "t"),
        P(ep, None, "t"),
        P(ep, None, "t"),
        P("t"),
    )
    return jax.shard_map(
        shards, mesh=split, in_specs=placed, out_specs=P(ep, "t"), check_vma=False
    )
```

```python
import jax
import jax.numpy as jnp
from jax import lax
from jax.experimental import pallas as pl
from jax.experimental.pallas import tpu as pltpu
from jax.sharding import Mesh, PartitionSpec as P


D = 2048
EXPERTS = 32
TOK = 128
CAP = 10
ROWS = EXPERTS * CAP
TP = 16
W = D // TP
HID = 224
EXTRA = 8
FRONT = ROWS + EXTRA
EPS = 1e-05

F32 = jnp.float32
BF16 = jnp.bfloat16
MIB = 1 << 20


def call(kernel, outs, mib, free=0, **kw):
    def run(*operands):
        near = operands[: len(operands) - free]
        far = operands[len(operands) - free :]
        many = isinstance(outs, list)
        vmem = pl.BlockSpec(memory_space=pltpu.VMEM)
        return pl.pallas_call(
            kernel,
            out_shape=[pltpu.VMEM(s, d) for s, d in outs] if many else pltpu.VMEM(*outs),
            in_specs=[vmem] * len(near) + [pl.BlockSpec(memory_space=pl.ANY)] * free,
            out_specs=[vmem] * len(outs) if many else vmem,
            compiler_params=pltpu.CompilerParams(vmem_limit_bytes=mib * MIB),
            **kw,
        )(*[pltpu.with_memory_space_constraint(x, pltpu.VMEM) for x in near], *far)

    return run


def place_of(slot, expert):
    return (slot // 2) * (2 * EXPERTS) + 2 * expert + slot % 2


def dispatch_kernel(routing_ref, tokens_ref, gain_ref, out_ref, place_ref, gain_out_ref):
    expert0, expert1 = routing_ref[0:1], routing_ref[1:2]
    index = lax.broadcasted_iota(jnp.int32, (EXPERTS, TOK), 0)
    hit0, hit1 = index == expert0, index == expert1
    both = jnp.where(hit0 | hit1, 1.0, 0.0).astype(BF16)
    earlier = jnp.where(
        lax.broadcasted_iota(jnp.int32, (TOK, TOK), 0)
        < lax.broadcasted_iota(jnp.int32, (TOK, TOK), 1),
        1.0,
        0.0,
    ).astype(BF16)
    before = jnp.dot(both, earlier, preferred_element_type=F32)
    slot0 = jnp.sum(jnp.where(hit0, before, 0.0), axis=0, keepdims=True).astype(jnp.int32)
    slot1 = jnp.sum(jnp.where(hit1, before, 0.0), axis=0, keepdims=True).astype(jnp.int32)
    place0, place1 = place_of(slot0, expert0), place_of(slot1, expert1)
    place_ref[0:1] = place0
    place_ref[1:2] = place1
    spots = lax.broadcasted_iota(jnp.int32, (ROWS, TOK), 0)
    picker = jnp.where((spots == place0) | (spots == place1), 1.0, 0.0).astype(BF16)
    rows = jnp.dot(picker, tokens_ref[...], preferred_element_type=F32).astype(BF16)
    for block in range(CAP // 2):
        piece = rows[block * 64 : (block + 1) * 64]
        out_ref[:, :, block * W : (block + 1) * W] = piece.reshape(EXPERTS, 2, W)
    gain = gain_ref[...]
    high = gain.astype(BF16).astype(F32)
    mid = (gain - high).astype(BF16).astype(F32)
    low = gain - high - mid
    part = lax.broadcasted_iota(jnp.int32, (EXTRA, W), 0)
    parts = jnp.where(part == 0, high, jnp.where(part == 1, mid, jnp.where(part == 2, low, 0.0)))
    gain_out_ref[...] = parts.astype(BF16)


def prepare_kernel(place_ref, weight_ref, pick_ref, weight_out_ref):
    spots = lax.broadcasted_iota(jnp.int32, (TOK, ROWS), 1).astype(F32)
    for k in range(2):
        place = jnp.broadcast_to(place_ref[k : k + 1].astype(F32), (TOK, TOK)).T
        pick_ref[k] = jnp.where(spots == place[:, 0:1], 1.0, 0.0).astype(BF16)
        weight_out_ref[k] = jnp.broadcast_to(weight_ref[k : k + 1], (TOK, TOK)).T


def spread_kernel(rows_ref, gain_ref, out_ref):
    gain = gain_ref[...]
    for block in range(CAP // 2):
        piece = rows_ref[:, :, block * W : (block + 1) * W].reshape(64, W)
        for peer in range(TP):
            out_ref[peer, block * 64 : (block + 1) * 64] = piece
    for peer in range(TP):
        out_ref[peer, ROWS:FRONT] = gain


def hidden_kernel(
    x_ref, gate_a, up_a, gate_far, up_far, out_ref, normed_ref, gate_b, up_b, sems
):
    copies = [
        pltpu.make_async_copy(gate_far, gate_b, sems.at[0]),
        pltpu.make_async_copy(up_far, up_b, sems.at[1]),
    ]
    for copy in copies:
        copy.start()
    total = jnp.zeros((ROWS, W), F32)
    for t in range(TP):
        piece = x_ref[t, :ROWS].astype(F32)
        total = total + piece * piece
    scale = lax.rsqrt(jnp.sum(total, axis=1, keepdims=True) / D + EPS)
    for t in range(TP):
        gain = jnp.sum(x_ref[t, ROWS:FRONT].astype(F32), axis=0, keepdims=True)
        piece = x_ref[t, :ROWS].astype(F32)
        normed_ref[:, t * W : (t + 1) * W] = (piece * scale * gain).astype(BF16)
    normed = normed_ref[...]
    across = (((1,), (1,)), ((), ()))

    def half(gate_ref, up_ref):
        gate = lax.dot_general(normed, gate_ref[...], across, preferred_element_type=F32)
        upper = lax.dot_general(normed, up_ref[...], across, preferred_element_type=F32)
        return (jax.nn.silu(gate) * upper).astype(BF16)

    out_ref[0] = half(gate_a, up_a)
    for copy in copies:
        copy.wait()
    out_ref[1] = half(gate_b, up_b)


def output_kernel(hidden_ref, down_a, down_b, out_ref):
    first, second = hidden_ref[0], hidden_ref[1]
    for t in range(TP):
        part = jnp.dot(first, down_a[t], preferred_element_type=F32)
        part = part + jnp.dot(second, down_b[t], preferred_element_type=F32)
        out_ref[t] = part.astype(BF16)


def reduce_kernel(parts_ref, out_ref):
    for block in range(CAP // 2):
        total = jnp.zeros((64, W), F32)
        for t in range(TP):
            total = total + parts_ref[t, block * 64 : (block + 1) * 64].astype(F32)
        out_ref[:, :, block * W : (block + 1) * W] = total.astype(BF16).reshape(EXPERTS, 2, W)


def combine_kernel(rows_ref, pick_ref, weight_ref, mixed_ref, square_ref):
    rows = jnp.concatenate(
        [
            rows_ref[:, :, block * W : (block + 1) * W].reshape(64, W)
            for block in range(CAP // 2)
        ],
        axis=0,
    )
    mixed = jnp.zeros((TOK, W), F32)
    for k in range(2):
        row = jnp.dot(pick_ref[k], rows, preferred_element_type=F32)
        mixed = mixed + row * weight_ref[k]
    mixed_ref[...] = mixed
    square = jnp.sum((mixed * mixed).T, axis=0, keepdims=True)
    for t in range(TP):
        square_ref[t] = square


def finish_kernel(mixed_ref, square_ref, gain_ref, out_ref):
    square = jnp.zeros((1, TOK), F32)
    for t in range(TP):
        square = square + square_ref[t]
    column = jnp.broadcast_to(lax.rsqrt(square / D + EPS), (TOK, TOK)).T
    out_ref[...] = (mixed_ref[...] * column * gain_ref[...]).astype(BF16)


def shards(
    tokens, norm_gain, routing, route_weight, gate_weight, up_weight, down_weight, final_gain
):
    swap = [(0, 1), (1, 0)]
    gate_own, up_own = gate_weight[0].T, up_weight[0].T
    outgoing, place, gain_parts = call(
        dispatch_kernel,
        [((EXPERTS, 2, 640), BF16), ((2, TOK), jnp.int32), ((EXTRA, W), BF16)],
        4,
    )(routing.T, tokens, norm_gain.reshape(1, W))
    arrived = lax.all_to_all(outgoing, "z", 0, 0, tiled=True)
    down_own = lax.all_to_all(down_weight.reshape(TP, HID, W), "t", 0, 0, tiled=True)
    gate_other = lax.ppermute(gate_own, "c", swap)
    up_other = lax.ppermute(up_own, "c", swap)
    down_other = lax.ppermute(down_own, "c", swap)
    pick, weight = call(
        prepare_kernel,
        [((2, TOK, ROWS), BF16), ((2, TOK, W), F32)],
        4,
    )(place, route_weight.T)
    spread = call(spread_kernel, ((TP, FRONT, W), BF16), 4)(arrived, gain_parts)
    features = lax.all_to_all(spread, "t", 0, 0, tiled=True)
    hidden = call(
        hidden_kernel,
        ((2, ROWS, HID), BF16),
        16,
        free=2,
        scratch_shapes=[
            pltpu.VMEM((ROWS, D), BF16),
            pltpu.VMEM((HID, D), BF16),
            pltpu.VMEM((HID, D), BF16),
            pltpu.SemaphoreType.DMA((2,)),
        ],
    )(features, gate_own, up_own, gate_other, up_other)
    parts = call(output_kernel, ((TP, ROWS, W), BF16), 8)(
        hidden, down_own, down_other
    )
    parts = lax.all_to_all(parts, "t", 0, 0, tiled=True)
    reduced = call(reduce_kernel, ((EXPERTS, 2, 640), BF16), 4)(parts)
    returned = lax.all_to_all(reduced, "z", 0, 0, tiled=True)
    mixed, square = call(
        combine_kernel, [((TOK, W), F32), ((TP, 1, TOK), F32)], 4
    )(returned, pick, weight)
    squares = lax.all_to_all(square, "t", 0, 0, tiled=True)
    return call(finish_kernel, ((TOK, W), BF16), 4)(mixed, squares, final_gain.reshape(1, W))


def solution(mesh):
    split = Mesh(mesh.devices.reshape(EXPERTS, 2, TP), ("z", "c", "t"))
    ep = ("z", "c")
    placed = (
        P(ep, "t"),
        P("t"),
        P(ep, None),
        P(ep, None),
        P(ep, None, "t"),
        P(ep, None, "t"),
        P(ep, None, "t"),
        P("t"),
    )
    return jax.shard_map(
        shards, mesh=split, in_specs=placed, out_specs=P(ep, "t"), check_vma=False
    )
```

```python
import jax
import jax.numpy as jnp
from jax import lax
from jax.experimental import pallas as pl
from jax.experimental.pallas import tpu as pltpu
from jax.sharding import Mesh, PartitionSpec as P


D = 2048
EXPERTS = 32
TOK = 128
CAP = 10
ROWS = EXPERTS * CAP
TP = 16
W = D // TP
HID = 224
EXTRA = 8
FIRST = 16
FRONT = ROWS + EXTRA
EPS = 1e-05

F32 = jnp.float32
BF16 = jnp.bfloat16
MIB = 1 << 20


def call(kernel, outs, mib, free=0, **kw):
    def run(*operands):
        near = operands[: len(operands) - free]
        far = operands[len(operands) - free :]
        many = isinstance(outs, list)
        vmem = pl.BlockSpec(memory_space=pltpu.VMEM)
        return pl.pallas_call(
            kernel,
            out_shape=[pltpu.VMEM(s, d) for s, d in outs] if many else pltpu.VMEM(*outs),
            in_specs=[vmem] * len(near) + [pl.BlockSpec(memory_space=pl.ANY)] * free,
            out_specs=[vmem] * len(outs) if many else vmem,
            compiler_params=pltpu.CompilerParams(vmem_limit_bytes=mib * MIB),
            **kw,
        )(*[pltpu.with_memory_space_constraint(x, pltpu.VMEM) for x in near], *far)

    return run


def place_of(slot, expert):
    position = (expert + EXPERTS - FIRST) % EXPERTS
    return (slot // 2) * (2 * EXPERTS) + 2 * position + slot % 2


def exchange(blocks):
    order = [(p + FIRST) % EXPERTS for p in range(EXPERTS)]
    return lax.all_to_all(blocks, "z", 0, 0, axis_index_groups=[order], tiled=True)


def dispatch_kernel(routing_ref, tokens_ref, gain_ref, out_ref, place_ref, gain_out_ref):
    expert0, expert1 = routing_ref[0:1], routing_ref[1:2]
    index = lax.broadcasted_iota(jnp.int32, (EXPERTS, TOK), 0)
    hit0, hit1 = index == expert0, index == expert1
    both = jnp.where(hit0 | hit1, 1.0, 0.0).astype(BF16)
    earlier = jnp.where(
        lax.broadcasted_iota(jnp.int32, (TOK, TOK), 0)
        < lax.broadcasted_iota(jnp.int32, (TOK, TOK), 1),
        1.0,
        0.0,
    ).astype(BF16)
    before = jnp.dot(both, earlier, preferred_element_type=F32)
    slot0 = jnp.sum(jnp.where(hit0, before, 0.0), axis=0, keepdims=True).astype(jnp.int32)
    slot1 = jnp.sum(jnp.where(hit1, before, 0.0), axis=0, keepdims=True).astype(jnp.int32)
    place0, place1 = place_of(slot0, expert0), place_of(slot1, expert1)
    place_ref[0:1] = place0
    place_ref[1:2] = place1
    spots = lax.broadcasted_iota(jnp.int32, (ROWS, TOK), 0)
    picker = jnp.where((spots == place0) | (spots == place1), 1.0, 0.0).astype(BF16)
    rows = jnp.dot(picker, tokens_ref[...], preferred_element_type=F32).astype(BF16)
    for block in range(CAP // 2):
        piece = rows[block * 64 : (block + 1) * 64]
        out_ref[:, :, block * W : (block + 1) * W] = piece.reshape(EXPERTS, 2, W)
    gain = gain_ref[...]
    high = gain.astype(BF16).astype(F32)
    mid = (gain - high).astype(BF16).astype(F32)
    low = gain - high - mid
    part = lax.broadcasted_iota(jnp.int32, (EXTRA, W), 0)
    parts = jnp.where(part == 0, high, jnp.where(part == 1, mid, jnp.where(part == 2, low, 0.0)))
    gain_out_ref[...] = parts.astype(BF16)


def prepare_kernel(place_ref, weight_ref, pick_ref, weight_out_ref):
    spots = lax.broadcasted_iota(jnp.int32, (TOK, ROWS), 1).astype(F32)
    for k in range(2):
        place = jnp.broadcast_to(place_ref[k : k + 1].astype(F32), (TOK, TOK)).T
        pick_ref[k] = jnp.where(spots == place[:, 0:1], 1.0, 0.0).astype(BF16)
        weight_out_ref[k] = jnp.broadcast_to(weight_ref[k : k + 1], (TOK, TOK)).T


def spread_kernel(rows_ref, gain_ref, down_ref, out_ref):
    gain = gain_ref[...]
    for block in range(CAP // 2):
        piece = rows_ref[:, :, block * W : (block + 1) * W].reshape(64, W)
        for peer in range(TP):
            out_ref[peer, block * 64 : (block + 1) * 64] = piece
    for peer in range(TP):
        out_ref[peer, ROWS:FRONT] = gain
        out_ref[peer, FRONT:] = down_ref[peer]


def hidden_kernel(
    x_ref, gate_a, up_a, gate_far, up_far, out_ref, normed_ref, gate_b, up_b, sems
):
    copies = [
        pltpu.make_async_copy(gate_far, gate_b, sems.at[0]),
        pltpu.make_async_copy(up_far, up_b, sems.at[1]),
    ]
    for copy in copies:
        copy.start()
    total = jnp.zeros((ROWS, W), F32)
    for t in range(TP):
        piece = x_ref[t, :ROWS].astype(F32)
        total = total + piece * piece
    scale = lax.rsqrt(jnp.sum(total, axis=1, keepdims=True) / D + EPS)
    for t in range(TP):
        gain = jnp.sum(x_ref[t, ROWS:FRONT].astype(F32), axis=0, keepdims=True)
        piece = x_ref[t, :ROWS].astype(F32)
        normed_ref[:, t * W : (t + 1) * W] = (piece * scale * gain).astype(BF16)
    normed = normed_ref[...]
    across = (((1,), (1,)), ((), ()))

    def half(gate_ref, up_ref):
        gate = lax.dot_general(normed, gate_ref[...], across, preferred_element_type=F32)
        upper = lax.dot_general(normed, up_ref[...], across, preferred_element_type=F32)
        return (jax.nn.silu(gate) * upper).astype(BF16)

    out_ref[0] = half(gate_a, up_a)
    for copy in copies:
        copy.wait()
    out_ref[1] = half(gate_b, up_b)


def output_kernel(hidden_ref, x_ref, down_ref, out_ref):
    first, second = hidden_ref[0], hidden_ref[1]
    for t in range(TP):
        part = jnp.dot(first, x_ref[t, FRONT:], preferred_element_type=F32)
        part = part + jnp.dot(second, down_ref[t], preferred_element_type=F32)
        out_ref[t] = part.astype(BF16)


def reduce_kernel(parts_ref, out_ref):
    for block in range(CAP // 2):
        total = jnp.zeros((64, W), F32)
        for t in range(TP):
            total = total + parts_ref[t, block * 64 : (block + 1) * 64].astype(F32)
        out_ref[:, :, block * W : (block + 1) * W] = total.astype(BF16).reshape(EXPERTS, 2, W)


def combine_kernel(rows_ref, pick_ref, weight_ref, mixed_ref, square_ref):
    rows = jnp.concatenate(
        [
            rows_ref[:, :, block * W : (block + 1) * W].reshape(64, W)
            for block in range(CAP // 2)
        ],
        axis=0,
    )
    mixed = jnp.zeros((TOK, W), F32)
    for k in range(2):
        row = jnp.dot(pick_ref[k], rows, preferred_element_type=F32)
        mixed = mixed + row * weight_ref[k]
    mixed_ref[...] = mixed
    square = jnp.sum((mixed * mixed).T, axis=0, keepdims=True)
    for t in range(TP):
        square_ref[t] = square


def finish_kernel(mixed_ref, square_ref, gain_ref, out_ref):
    square = jnp.zeros((1, TOK), F32)
    for t in range(TP):
        square = square + square_ref[t]
    column = jnp.broadcast_to(lax.rsqrt(square / D + EPS), (TOK, TOK)).T
    out_ref[...] = (mixed_ref[...] * column * gain_ref[...]).astype(BF16)


def shards(
    tokens, norm_gain, routing, route_weight, gate_weight, up_weight, down_weight, final_gain
):
    swap = [(0, 1), (1, 0)]
    gate_own, up_own = gate_weight[0].T, up_weight[0].T
    outgoing, place, gain_parts = call(
        dispatch_kernel,
        [((EXPERTS, 2, 640), BF16), ((2, TOK), jnp.int32), ((EXTRA, W), BF16)],
        4,
    )(routing.T, tokens, norm_gain.reshape(1, W))
    arrived = exchange(outgoing)
    gate_other = lax.ppermute(gate_own, "c", swap)
    up_other = lax.ppermute(up_own, "c", swap)
    pick, weight = call(
        prepare_kernel,
        [((2, TOK, ROWS), BF16), ((2, TOK, W), F32)],
        4,
    )(place, route_weight.T)
    spread = call(spread_kernel, ((TP, FRONT + HID, W), BF16), 4)(
        arrived, gain_parts, down_weight.reshape(TP, HID, W)
    )
    features = lax.all_to_all(spread, "t", 0, 0, tiled=True)
    down_other = lax.ppermute(features[:, FRONT:], "c", swap)
    hidden = call(
        hidden_kernel,
        ((2, ROWS, HID), BF16),
        16,
        free=2,
        scratch_shapes=[
            pltpu.VMEM((ROWS, D), BF16),
            pltpu.VMEM((HID, D), BF16),
            pltpu.VMEM((HID, D), BF16),
            pltpu.SemaphoreType.DMA((2,)),
        ],
    )(features, gate_own, up_own, gate_other, up_other)
    parts = call(output_kernel, ((TP, ROWS, W), BF16), 8)(
        hidden, features, down_other
    )
    parts = lax.all_to_all(parts, "t", 0, 0, tiled=True)
    reduced = call(reduce_kernel, ((EXPERTS, 2, 640), BF16), 4)(parts)
    returned = exchange(reduced)
    mixed, square = call(
        combine_kernel, [((TOK, W), F32), ((TP, 1, TOK), F32)], 4
    )(returned, pick, weight)
    squares = lax.all_to_all(square, "t", 0, 0, tiled=True)
    return call(finish_kernel, ((TOK, W), BF16), 4)(mixed, squares, final_gain.reshape(1, W))


def solution(mesh):
    split = Mesh(mesh.devices.reshape(EXPERTS, 2, TP), ("z", "c", "t"))
    ep = ("z", "c")
    placed = (
        P(ep, "t"),
        P("t"),
        P(ep, None),
        P(ep, None),
        P(ep, None, "t"),
        P(ep, None, "t"),
        P(ep, None, "t"),
        P("t"),
    )
    return jax.shard_map(
        shards, mesh=split, in_specs=placed, out_specs=P(ep, "t"), check_vma=False
    )
```

```python
import jax
import jax.numpy as jnp
from jax import lax
from jax.experimental import pallas as pl
from jax.experimental.pallas import tpu as pltpu
from jax.sharding import Mesh, PartitionSpec as P


D = 2048
EXPERTS = 32
TOK = 128
CAP = 10
ROWS = EXPERTS * CAP
TP = 16
W = D // TP
HID = 224
EXTRA = 8
FIRST = 16
FRONT = ROWS + EXTRA
EPS = 1e-05

F32 = jnp.float32
BF16 = jnp.bfloat16
MIB = 1 << 20


def call(kernel, outs, mib, hbm=0, **kw):
    def run(*operands):
        many = isinstance(outs, list)
        near = len(operands) - hbm
        vmem = pl.BlockSpec(memory_space=pltpu.VMEM)
        spaces = [pltpu.VMEM] * near + [pltpu.HBM] * hbm
        return pl.pallas_call(
            kernel,
            out_shape=[pltpu.VMEM(s, d) for s, d in outs] if many else pltpu.VMEM(*outs),
            in_specs=[pl.BlockSpec(memory_space=space) for space in spaces],
            out_specs=[vmem] * len(outs) if many else vmem,
            compiler_params=pltpu.CompilerParams(vmem_limit_bytes=mib * MIB),
            **kw,
        )(
            *[
                pltpu.with_memory_space_constraint(x, space)
                for x, space in zip(operands, spaces)
            ]
        )

    return run


def place_of(slot, expert):
    position = (expert + EXPERTS - FIRST) % EXPERTS
    return (slot // 2) * (2 * EXPERTS) + 2 * position + slot % 2


def exchange(blocks):
    order = [(p + FIRST) % EXPERTS for p in range(EXPERTS)]
    return lax.all_to_all(blocks, "z", 0, 0, axis_index_groups=[order], tiled=True)


def dispatch_kernel(
    routing_far, tokens_far, gain_far, out_ref, place_ref, gain_out_ref,
    routing_ref, tokens_ref, gain_ref, sems,
):
    copies = [
        pltpu.make_async_copy(routing_far, routing_ref, sems.at[0]),
        pltpu.make_async_copy(tokens_far, tokens_ref, sems.at[1]),
        pltpu.make_async_copy(gain_far, gain_ref, sems.at[2]),
    ]
    for copy in copies:
        copy.start()
    copies[0].wait()
    expert0, expert1 = routing_ref[0:1], routing_ref[1:2]
    index = lax.broadcasted_iota(jnp.int32, (EXPERTS, TOK), 0)
    hit0, hit1 = index == expert0, index == expert1
    both = jnp.where(hit0 | hit1, 1.0, 0.0).astype(BF16)
    earlier = jnp.where(
        lax.broadcasted_iota(jnp.int32, (TOK, TOK), 0)
        < lax.broadcasted_iota(jnp.int32, (TOK, TOK), 1),
        1.0,
        0.0,
    ).astype(BF16)
    before = jnp.dot(both, earlier, preferred_element_type=F32)
    slot0 = jnp.sum(jnp.where(hit0, before, 0.0), axis=0, keepdims=True).astype(jnp.int32)
    slot1 = jnp.sum(jnp.where(hit1, before, 0.0), axis=0, keepdims=True).astype(jnp.int32)
    place0, place1 = place_of(slot0, expert0), place_of(slot1, expert1)
    place_ref[0:1] = place0
    place_ref[1:2] = place1
    spots = lax.broadcasted_iota(jnp.int32, (ROWS, TOK), 0)
    picker = jnp.where((spots == place0) | (spots == place1), 1.0, 0.0).astype(BF16)
    copies[1].wait()
    rows = jnp.dot(picker, tokens_ref[...], preferred_element_type=F32).astype(BF16)
    for block in range(CAP // 2):
        piece = rows[block * 64 : (block + 1) * 64]
        out_ref[:, :, block * W : (block + 1) * W] = piece.reshape(EXPERTS, 2, W)
    copies[2].wait()
    gain = gain_ref[...]
    high = gain.astype(BF16).astype(F32)
    mid = (gain - high).astype(BF16).astype(F32)
    low = gain - high - mid
    part = lax.broadcasted_iota(jnp.int32, (EXTRA, W), 0)
    parts = jnp.where(part == 0, high, jnp.where(part == 1, mid, jnp.where(part == 2, low, 0.0)))
    gain_out_ref[...] = parts.astype(BF16)


def prepare_kernel(place_ref, weight_ref, pick_ref, weight_out_ref):
    spots = lax.broadcasted_iota(jnp.int32, (TOK, ROWS), 1).astype(F32)
    for k in range(2):
        place = jnp.broadcast_to(place_ref[k : k + 1].astype(F32), (TOK, TOK)).T
        pick_ref[k] = jnp.where(spots == place[:, 0:1], 1.0, 0.0).astype(BF16)
        weight_out_ref[k] = jnp.broadcast_to(weight_ref[k : k + 1], (TOK, TOK)).T


def spread_kernel(rows_ref, gain_ref, down_far, out_ref, sem):
    down = pltpu.make_async_copy(down_far, out_ref.at[:, FRONT:], sem)
    down.start()
    gain = gain_ref[...]
    for block in range(CAP // 2):
        piece = rows_ref[:, :, block * W : (block + 1) * W].reshape(64, W)
        for peer in range(TP):
            out_ref[peer, block * 64 : (block + 1) * 64] = piece
    for peer in range(TP):
        out_ref[peer, ROWS:FRONT] = gain
    down.wait()


def hidden_kernel(x_ref, gate_a, gate_b, up_a, up_b, out_ref, normed_ref):
    total = jnp.zeros((ROWS, W), F32)
    for t in range(TP):
        piece = x_ref[t, :ROWS].astype(F32)
        total = total + piece * piece
    scale = lax.rsqrt(jnp.sum(total, axis=1, keepdims=True) / D + EPS)
    for t in range(TP):
        gain = jnp.sum(x_ref[t, ROWS:FRONT].astype(F32), axis=0, keepdims=True)
        piece = x_ref[t, :ROWS].astype(F32)
        normed_ref[:, t * W : (t + 1) * W] = (piece * scale * gain).astype(BF16)
    normed = normed_ref[...]
    across = (((1,), (1,)), ((), ()))
    for half, (gate_ref, up_ref) in enumerate(((gate_a, up_a), (gate_b, up_b))):
        gate = lax.dot_general(normed, gate_ref[...], across, preferred_element_type=F32)
        upper = lax.dot_general(normed, up_ref[...], across, preferred_element_type=F32)
        out_ref[half] = (jax.nn.silu(gate) * upper).astype(BF16)


def output_kernel(hidden_ref, x_ref, down_ref, out_ref):
    first, second = hidden_ref[0], hidden_ref[1]
    for t in range(0, TP, 2):
        own = jnp.concatenate([x_ref[t, FRONT:], x_ref[t + 1, FRONT:]], axis=1)
        other = jnp.concatenate([down_ref[t], down_ref[t + 1]], axis=1)
        part = jnp.dot(first, own, preferred_element_type=F32)
        part = (part + jnp.dot(second, other, preferred_element_type=F32)).astype(BF16)
        out_ref[t] = part[:, :W]
        out_ref[t + 1] = part[:, W:]


def reduce_kernel(parts_ref, out_ref):
    for block in range(CAP // 2):
        total = jnp.zeros((64, W), F32)
        for t in range(TP):
            total = total + parts_ref[t, block * 64 : (block + 1) * 64].astype(F32)
        out_ref[:, :, block * W : (block + 1) * W] = total.astype(BF16).reshape(EXPERTS, 2, W)


def combine_kernel(rows_ref, pick_ref, weight_ref, mixed_ref, square_ref):
    rows = jnp.concatenate(
        [
            rows_ref[:, :, block * W : (block + 1) * W].reshape(64, W)
            for block in range(CAP // 2)
        ],
        axis=0,
    )
    mixed = jnp.zeros((TOK, W), F32)
    for k in range(2):
        row = jnp.dot(pick_ref[k], rows, preferred_element_type=F32)
        mixed = mixed + row * weight_ref[k]
    mixed_ref[...] = mixed
    square = jnp.sum((mixed * mixed).T, axis=0, keepdims=True)
    for t in range(TP):
        square_ref[t] = square


def finish_kernel(mixed_ref, square_ref, gain_ref, out_ref):
    square = jnp.zeros((1, TOK), F32)
    for t in range(TP):
        square = square + square_ref[t]
    column = jnp.broadcast_to(lax.rsqrt(square / D + EPS), (TOK, TOK)).T
    out_ref[...] = (mixed_ref[...] * column * gain_ref[...]).astype(BF16)


def shards(
    tokens, norm_gain, routing, route_weight, gate_weight, up_weight, down_weight, final_gain
):
    swap = [(0, 1), (1, 0)]
    gate_own, up_own = gate_weight[0].T, up_weight[0].T
    outgoing, place, gain_parts = call(
        dispatch_kernel,
        [((EXPERTS, 2, 640), BF16), ((2, TOK), jnp.int32), ((EXTRA, W), BF16)],
        4,
        hbm=3,
        scratch_shapes=[
            pltpu.VMEM((2, TOK), jnp.int32),
            pltpu.VMEM((TOK, W), BF16),
            pltpu.VMEM((1, W), F32),
            pltpu.SemaphoreType.DMA((3,)),
        ],
    )(routing.T, tokens, norm_gain.reshape(1, W))
    arrived = exchange(outgoing)
    gate_other = lax.ppermute(gate_own, "c", swap)
    up_other = lax.ppermute(up_own, "c", swap)
    pick, weight = call(
        prepare_kernel,
        [((2, TOK, ROWS), BF16), ((2, TOK, W), F32)],
        4,
    )(place, route_weight.T)
    spread = call(
        spread_kernel,
        ((TP, FRONT + HID, W), BF16),
        4,
        hbm=1,
        scratch_shapes=[pltpu.SemaphoreType.DMA],
    )(
        arrived, gain_parts, down_weight.reshape(TP, HID, W)
    )
    features = lax.all_to_all(spread, "t", 0, 0, tiled=True)
    down_other = lax.ppermute(features[:, FRONT:], "c", swap)
    hidden = call(
        hidden_kernel,
        ((2, ROWS, HID), BF16),
        16,
        scratch_shapes=[pltpu.VMEM((ROWS, D), BF16)],
    )(features, gate_own, gate_other, up_own, up_other)
    parts = call(output_kernel, ((TP, ROWS, W), BF16), 8)(
        hidden, features, down_other
    )
    parts = lax.all_to_all(parts, "t", 0, 0, tiled=True)
    reduced = call(reduce_kernel, ((EXPERTS, 2, 640), BF16), 4)(parts)
    returned = exchange(reduced)
    mixed, square = call(
        combine_kernel, [((TOK, W), F32), ((TP, 1, TOK), F32)], 4
    )(returned, pick, weight)
    squares = lax.all_to_all(square, "t", 0, 0, tiled=True)
    return call(finish_kernel, ((TOK, W), BF16), 4)(mixed, squares, final_gain.reshape(1, W))


def solution(mesh):
    split = Mesh(mesh.devices.reshape(EXPERTS, 2, TP), ("z", "c", "t"))
    ep = ("z", "c")
    placed = (
        P(ep, "t"),
        P("t"),
        P(ep, None),
        P(ep, None),
        P(ep, None, "t"),
        P(ep, None, "t"),
        P(ep, None, "t"),
        P("t"),
    )
    return jax.shard_map(
        shards, mesh=split, in_specs=placed, out_specs=P(ep, "t"), check_vma=False
    )
```

```python
import jax
import jax.numpy as jnp
from jax import lax
from jax.experimental import pallas as pl
from jax.experimental.pallas import tpu as pltpu
from jax.sharding import Mesh, PartitionSpec as P


D = 2048
EXPERTS = 32
TOK = 128
CAP = 10
ROWS = EXPERTS * CAP
TP = 16
W = D // TP
HID = 224
EXTRA = 8
FIRST = 16
FIRST_TP = 10
FRONT = ROWS + EXTRA
EPS = 1e-05

F32 = jnp.float32
BF16 = jnp.bfloat16
MIB = 1 << 20


def call(kernel, outs, mib, hbm=0, **kw):
    def run(*operands):
        many = isinstance(outs, list)
        near = len(operands) - hbm
        vmem = pl.BlockSpec(memory_space=pltpu.VMEM)
        spaces = [pltpu.VMEM] * near + [pltpu.HBM] * hbm
        return pl.pallas_call(
            kernel,
            out_shape=[pltpu.VMEM(s, d) for s, d in outs] if many else pltpu.VMEM(*outs),
            in_specs=[pl.BlockSpec(memory_space=space) for space in spaces],
            out_specs=[vmem] * len(outs) if many else vmem,
            compiler_params=pltpu.CompilerParams(vmem_limit_bytes=mib * MIB),
            **kw,
        )(
            *[
                pltpu.with_memory_space_constraint(x, space)
                for x, space in zip(operands, spaces)
            ]
        )

    return run


def place_of(slot, expert):
    position = (expert + EXPERTS - FIRST) % EXPERTS
    return (slot // 2) * (2 * EXPERTS) + 2 * position + slot % 2


def exchange(blocks):
    order = [(p + FIRST) % EXPERTS for p in range(EXPERTS)]
    return lax.all_to_all(blocks, "z", 0, 0, axis_index_groups=[order], tiled=True)


def across_plane(blocks):
    order = [p ^ FIRST_TP for p in range(TP)]
    return lax.all_to_all(blocks, "t", 0, 0, axis_index_groups=[order], tiled=True)


def dispatch_kernel(
    routing_far, tokens_far, gain_far, out_ref, place_ref, gain_out_ref,
    routing_ref, tokens_ref, gain_ref, sems,
):
    copies = [
        pltpu.make_async_copy(routing_far, routing_ref, sems.at[0]),
        pltpu.make_async_copy(tokens_far, tokens_ref, sems.at[1]),
        pltpu.make_async_copy(gain_far, gain_ref, sems.at[2]),
    ]
    for copy in copies:
        copy.start()
    copies[0].wait()
    expert0, expert1 = routing_ref[0:1], routing_ref[1:2]
    index = lax.broadcasted_iota(jnp.int32, (EXPERTS, TOK), 0)
    hit0, hit1 = index == expert0, index == expert1
    both = jnp.where(hit0 | hit1, 1.0, 0.0).astype(BF16)
    earlier = jnp.where(
        lax.broadcasted_iota(jnp.int32, (TOK, TOK), 0)
        < lax.broadcasted_iota(jnp.int32, (TOK, TOK), 1),
        1.0,
        0.0,
    ).astype(BF16)
    before = jnp.dot(both, earlier, preferred_element_type=F32)
    slot0 = jnp.sum(jnp.where(hit0, before, 0.0), axis=0, keepdims=True).astype(jnp.int32)
    slot1 = jnp.sum(jnp.where(hit1, before, 0.0), axis=0, keepdims=True).astype(jnp.int32)
    place0, place1 = place_of(slot0, expert0), place_of(slot1, expert1)
    place_ref[0:1] = place0
    place_ref[1:2] = place1
    spots = lax.broadcasted_iota(jnp.int32, (ROWS, TOK), 0)
    picker = jnp.where((spots == place0) | (spots == place1), 1.0, 0.0).astype(BF16)
    copies[1].wait()
    rows = jnp.dot(picker, tokens_ref[...], preferred_element_type=F32).astype(BF16)
    for block in range(CAP // 2):
        piece = rows[block * 64 : (block + 1) * 64]
        out_ref[:, :, block * W : (block + 1) * W] = piece.reshape(EXPERTS, 2, W)
    copies[2].wait()
    gain = gain_ref[...]
    high = gain.astype(BF16).astype(F32)
    mid = (gain - high).astype(BF16).astype(F32)
    low = gain - high - mid
    part = lax.broadcasted_iota(jnp.int32, (EXTRA, W), 0)
    parts = jnp.where(part == 0, high, jnp.where(part == 1, mid, jnp.where(part == 2, low, 0.0)))
    gain_out_ref[...] = parts.astype(BF16)


def prepare_kernel(place_ref, weight_ref, pick_ref, weight_out_ref):
    spots = lax.broadcasted_iota(jnp.int32, (TOK, ROWS), 1).astype(F32)
    for k in range(2):
        place = jnp.broadcast_to(place_ref[k : k + 1].astype(F32), (TOK, TOK)).T
        pick_ref[k] = jnp.where(spots == place[:, 0:1], 1.0, 0.0).astype(BF16)
        weight_out_ref[k] = jnp.broadcast_to(weight_ref[k : k + 1], (TOK, TOK)).T


def spread_kernel(rows_ref, gain_ref, down_far, out_ref, sems):
    copies = [
        pltpu.make_async_copy(
            down_far.at[peer ^ FIRST_TP], out_ref.at[peer, FRONT:], sems.at[peer]
        )
        for peer in range(TP)
    ]
    for copy in copies:
        copy.start()
    gain = gain_ref[...]
    for block in range(CAP // 2):
        piece = rows_ref[:, :, block * W : (block + 1) * W].reshape(64, W)
        for peer in range(TP):
            out_ref[peer, block * 64 : (block + 1) * 64] = piece
    for peer in range(TP):
        out_ref[peer, ROWS:FRONT] = gain
    for copy in copies:
        copy.wait()


def hidden_kernel(x_ref, gate_a, gate_b, up_a, up_b, out_ref, normed_ref):
    total = jnp.zeros((ROWS, W), F32)
    for t in range(TP):
        piece = x_ref[t, :ROWS].astype(F32)
        total = total + piece * piece
    scale = lax.rsqrt(jnp.sum(total, axis=1, keepdims=True) / D + EPS)
    for p in range(TP):
        gain = jnp.sum(x_ref[p, ROWS:FRONT].astype(F32), axis=0, keepdims=True)
        piece = x_ref[p, :ROWS].astype(F32)
        t = p ^ FIRST_TP
        normed_ref[:, t * W : (t + 1) * W] = (piece * scale * gain).astype(BF16)
    normed = normed_ref[...]
    across = (((1,), (1,)), ((), ()))
    for half, (gate_ref, up_ref) in enumerate(((gate_a, up_a), (gate_b, up_b))):
        gate = lax.dot_general(normed, gate_ref[...], across, preferred_element_type=F32)
        upper = lax.dot_general(normed, up_ref[...], across, preferred_element_type=F32)
        out_ref[half] = (jax.nn.silu(gate) * upper).astype(BF16)


def output_kernel(hidden_ref, x_ref, down_ref, out_ref):
    first, second = hidden_ref[0], hidden_ref[1]
    for t in range(0, TP, 2):
        own = jnp.concatenate([x_ref[t, FRONT:], x_ref[t + 1, FRONT:]], axis=1)
        other = jnp.concatenate([down_ref[t], down_ref[t + 1]], axis=1)
        part = jnp.dot(first, own, preferred_element_type=F32)
        part = (part + jnp.dot(second, other, preferred_element_type=F32)).astype(BF16)
        out_ref[t] = part[:, :W]
        out_ref[t + 1] = part[:, W:]


def reduce_kernel(parts_ref, out_ref):
    for block in range(CAP // 2):
        total = jnp.zeros((64, W), F32)
        for t in range(TP):
            total = total + parts_ref[t, block * 64 : (block + 1) * 64].astype(F32)
        out_ref[:, :, block * W : (block + 1) * W] = total.astype(BF16).reshape(EXPERTS, 2, W)


def combine_kernel(rows_ref, pick_ref, weight_ref, mixed_ref, square_ref):
    rows = jnp.concatenate(
        [
            rows_ref[:, :, block * W : (block + 1) * W].reshape(64, W)
            for block in range(CAP // 2)
        ],
        axis=0,
    )
    mixed = jnp.zeros((TOK, W), F32)
    for k in range(2):
        row = jnp.dot(pick_ref[k], rows, preferred_element_type=F32)
        mixed = mixed + row * weight_ref[k]
    mixed_ref[...] = mixed
    square = jnp.sum((mixed * mixed).T, axis=0, keepdims=True)
    for t in range(TP):
        square_ref[t] = square


def finish_kernel(mixed_ref, square_ref, gain_ref, out_ref):
    square = jnp.zeros((1, TOK), F32)
    for t in range(TP):
        square = square + square_ref[t]
    column = jnp.broadcast_to(lax.rsqrt(square / D + EPS), (TOK, TOK)).T
    out_ref[...] = (mixed_ref[...] * column * gain_ref[...]).astype(BF16)


def shards(
    tokens, norm_gain, routing, route_weight, gate_weight, up_weight, down_weight, final_gain
):
    swap = [(0, 1), (1, 0)]
    gate_own, up_own = gate_weight[0].T, up_weight[0].T
    outgoing, place, gain_parts = call(
        dispatch_kernel,
        [((EXPERTS, 2, 640), BF16), ((2, TOK), jnp.int32), ((EXTRA, W), BF16)],
        4,
        hbm=3,
        scratch_shapes=[
            pltpu.VMEM((2, TOK), jnp.int32),
            pltpu.VMEM((TOK, W), BF16),
            pltpu.VMEM((1, W), F32),
            pltpu.SemaphoreType.DMA((3,)),
        ],
    )(routing.T, tokens, norm_gain.reshape(1, W))
    arrived = exchange(outgoing)
    gate_other = lax.ppermute(gate_own, "c", swap)
    up_other = lax.ppermute(up_own, "c", swap)
    pick, weight = call(
        prepare_kernel,
        [((2, TOK, ROWS), BF16), ((2, TOK, W), F32)],
        4,
    )(place, route_weight.T)
    spread = call(
        spread_kernel,
        ((TP, FRONT + HID, W), BF16),
        4,
        hbm=1,
        scratch_shapes=[pltpu.SemaphoreType.DMA((TP,))],
    )(
        arrived, gain_parts, down_weight.reshape(TP, HID, W)
    )
    features = across_plane(spread)
    down_other = lax.ppermute(features[:, FRONT:], "c", swap)
    hidden = call(
        hidden_kernel,
        ((2, ROWS, HID), BF16),
        16,
        scratch_shapes=[pltpu.VMEM((ROWS, D), BF16)],
    )(features, gate_own, gate_other, up_own, up_other)
    parts = call(output_kernel, ((TP, ROWS, W), BF16), 8)(
        hidden, features, down_other
    )
    parts = across_plane(parts)
    reduced = call(reduce_kernel, ((EXPERTS, 2, 640), BF16), 4)(parts)
    returned = exchange(reduced)
    mixed, square = call(
        combine_kernel, [((TOK, W), F32), ((TP, 1, TOK), F32)], 4
    )(returned, pick, weight)
    squares = across_plane(square)
    return call(finish_kernel, ((TOK, W), BF16), 4)(mixed, squares, final_gain.reshape(1, W))


def solution(mesh):
    split = Mesh(mesh.devices.reshape(EXPERTS, 2, TP), ("z", "c", "t"))
    ep = ("z", "c")
    placed = (
        P(ep, "t"),
        P("t"),
        P(ep, None),
        P(ep, None),
        P(ep, None, "t"),
        P(ep, None, "t"),
        P(ep, None, "t"),
        P("t"),
    )
    return jax.shard_map(
        shards, mesh=split, in_specs=placed, out_specs=P(ep, "t"), check_vma=False
    )
```

```python
import jax
import jax.numpy as jnp
from jax import lax
from jax.experimental import pallas as pl
from jax.experimental.pallas import tpu as pltpu
from jax.sharding import Mesh, PartitionSpec as P


D = 2048
EXPERTS = 32
TOK = 128
CAP = 10
ROWS = EXPERTS * CAP
TP = 16
W = D // TP
HID = 224
EXTRA = 8
FIRST = 20
BACK = 18
FIRST_TP = 10
TURN = (BACK - FIRST) % EXPERTS
FRONT = ROWS + EXTRA
EPS = 1e-05

F32 = jnp.float32
BF16 = jnp.bfloat16
MIB = 1 << 20


def call(kernel, outs, mib, hbm=0, far_out=False, **kw):
    def run(*operands):
        many = isinstance(outs, list)
        near = len(operands) - hbm
        kept = [pltpu.HBM if far_out else pltpu.VMEM] + [pltpu.VMEM] * (len(outs) - 1)
        vmem = pl.BlockSpec(memory_space=pltpu.VMEM)
        spaces = [pltpu.VMEM] * near + [pltpu.HBM] * hbm
        return pl.pallas_call(
            kernel,
            out_shape=[s(*out) for s, out in zip(kept, outs)] if many else pltpu.VMEM(*outs),
            in_specs=[pl.BlockSpec(memory_space=space) for space in spaces],
            out_specs=[pl.BlockSpec(memory_space=s) for s in kept] if many else vmem,
            compiler_params=pltpu.CompilerParams(vmem_limit_bytes=mib * MIB),
            **kw,
        )(
            *[
                pltpu.with_memory_space_constraint(x, space)
                for x, space in zip(operands, spaces)
            ]
        )

    return run


def place_of(slot, expert):
    position = (expert + EXPERTS - FIRST) % EXPERTS
    return (slot // 2) * (2 * EXPERTS) + 2 * position + slot % 2


def exchange(blocks, first):
    order = [(p + first) % EXPERTS for p in range(EXPERTS)]
    return lax.all_to_all(blocks, "z", 0, 0, axis_index_groups=[order], tiled=True)


def across_plane(blocks):
    order = [p ^ FIRST_TP for p in range(TP)]
    return lax.all_to_all(blocks, "t", 0, 0, axis_index_groups=[order], tiled=True)


def dispatch_kernel(
    routing_far, tokens_far, gain_far, out_ref, place_ref, gain_out_ref,
    routing_ref, tokens_ref, gain_ref, rows_ref, sems,
):
    copies = [
        pltpu.make_async_copy(routing_far, routing_ref, sems.at[0]),
        pltpu.make_async_copy(tokens_far, tokens_ref, sems.at[1]),
        pltpu.make_async_copy(gain_far, gain_ref, sems.at[2]),
    ]
    for copy in copies:
        copy.start()
    copies[0].wait()
    expert0, expert1 = routing_ref[0:1], routing_ref[1:2]
    index = lax.broadcasted_iota(jnp.int32, (EXPERTS, TOK), 0)
    hit0, hit1 = index == expert0, index == expert1
    both = jnp.where(hit0 | hit1, 1.0, 0.0).astype(BF16)
    earlier = jnp.where(
        lax.broadcasted_iota(jnp.int32, (TOK, TOK), 0)
        < lax.broadcasted_iota(jnp.int32, (TOK, TOK), 1),
        1.0,
        0.0,
    ).astype(BF16)
    before = jnp.dot(both, earlier, preferred_element_type=F32)
    slot0 = jnp.sum(jnp.where(hit0, before, 0.0), axis=0, keepdims=True).astype(jnp.int32)
    slot1 = jnp.sum(jnp.where(hit1, before, 0.0), axis=0, keepdims=True).astype(jnp.int32)
    place0, place1 = place_of(slot0, expert0), place_of(slot1, expert1)
    spots = lax.broadcasted_iota(jnp.int32, (ROWS, TOK), 0)
    picker = jnp.where((spots == place0) | (spots == place1), 1.0, 0.0).astype(BF16)
    copies[1].wait()
    rows = jnp.dot(picker, tokens_ref[...], preferred_element_type=F32).astype(BF16)
    for block in range(CAP // 2):
        piece = rows[block * 64 : (block + 1) * 64]
        rows_ref[:, :, block * W : (block + 1) * W] = piece.reshape(EXPERTS, 2, W)
    sent = pltpu.make_async_copy(rows_ref, out_ref, sems.at[3])
    sent.start()
    place_ref[0:1] = place0
    place_ref[1:2] = place1
    copies[2].wait()
    gain = gain_ref[...]
    high = gain.astype(BF16).astype(F32)
    mid = (gain - high).astype(BF16).astype(F32)
    low = gain - high - mid
    part = lax.broadcasted_iota(jnp.int32, (EXTRA, W), 0)
    parts = jnp.where(part == 0, high, jnp.where(part == 1, mid, jnp.where(part == 2, low, 0.0)))
    gain_out_ref[...] = parts.astype(BF16)
    sent.wait()


def prepare_kernel(place_ref, weight_ref, pick_ref, weight_out_ref):
    spots = lax.broadcasted_iota(jnp.int32, (TOK, ROWS), 1).astype(F32)
    for k in range(2):
        place = jnp.broadcast_to(place_ref[k : k + 1].astype(F32), (TOK, TOK)).T
        pick_ref[k] = jnp.where(spots == place[:, 0:1], 1.0, 0.0).astype(BF16)
        weight_out_ref[k] = jnp.broadcast_to(weight_ref[k : k + 1], (TOK, TOK)).T


def spread_kernel(rows_ref, gain_ref, down_far, out_ref, sems):
    copies = [
        pltpu.make_async_copy(
            down_far.at[peer ^ FIRST_TP], out_ref.at[peer, FRONT:], sems.at[peer]
        )
        for peer in range(TP)
    ]
    for copy in copies:
        copy.start()
    gain = gain_ref[...]
    for block in range(CAP // 2):
        piece = rows_ref[:, :, block * W : (block + 1) * W].reshape(64, W)
        for peer in range(TP):
            out_ref[peer, block * 64 : (block + 1) * 64] = piece
    for peer in range(TP):
        out_ref[peer, ROWS:FRONT] = gain
    for copy in copies:
        copy.wait()


def hidden_kernel(x_ref, gate_a, gate_b, up_a, up_b, out_ref, normed_ref):
    total = jnp.zeros((ROWS, W), F32)
    for t in range(TP):
        piece = x_ref[t, :ROWS].astype(F32)
        total = total + piece * piece
    scale = lax.rsqrt(jnp.sum(total, axis=1, keepdims=True) / D + EPS)
    for p in range(TP):
        gain = jnp.sum(x_ref[p, ROWS:FRONT].astype(F32), axis=0, keepdims=True)
        piece = x_ref[p, :ROWS].astype(F32)
        t = p ^ FIRST_TP
        normed_ref[:, t * W : (t + 1) * W] = (piece * scale * gain).astype(BF16)
    normed = normed_ref[...]
    across = (((1,), (1,)), ((), ()))
    for half, (gate_ref, up_ref) in enumerate(((gate_a, up_a), (gate_b, up_b))):
        gate = lax.dot_general(normed, gate_ref[...], across, preferred_element_type=F32)
        upper = lax.dot_general(normed, up_ref[...], across, preferred_element_type=F32)
        out_ref[half] = (jax.nn.silu(gate) * upper).astype(BF16)


def output_kernel(hidden_ref, x_ref, down_ref, out_ref):
    first, second = hidden_ref[0], hidden_ref[1]
    for t in range(0, TP, 2):
        own = jnp.concatenate([x_ref[t, FRONT:], x_ref[t + 1, FRONT:]], axis=1)
        other = jnp.concatenate([down_ref[t], down_ref[t + 1]], axis=1)
        part = jnp.dot(first, own, preferred_element_type=F32)
        part = (part + jnp.dot(second, other, preferred_element_type=F32)).astype(BF16)
        out_ref[t] = part[:, :W]
        out_ref[t + 1] = part[:, W:]


def reduce_kernel(parts_ref, out_ref):
    for block in range(CAP // 2):
        total = jnp.zeros((64, W), F32)
        for t in range(TP):
            total = total + parts_ref[t, block * 64 : (block + 1) * 64].astype(F32)
        piece = total.astype(BF16).reshape(EXPERTS, 2, W)
        out_ref[: EXPERTS - TURN, :, block * W : (block + 1) * W] = piece[TURN:]
        out_ref[EXPERTS - TURN :, :, block * W : (block + 1) * W] = piece[:TURN]


def combine_kernel(rows_ref, pick_ref, weight_ref, mixed_ref, square_ref):
    rows = jnp.concatenate(
        [
            jnp.concatenate(
                [
                    rows_ref[EXPERTS - TURN :, :, block * W : (block + 1) * W],
                    rows_ref[: EXPERTS - TURN, :, block * W : (block + 1) * W],
                ]
            ).reshape(64, W)
            for block in range(CAP // 2)
        ],
        axis=0,
    )
    mixed = jnp.zeros((TOK, W), F32)
    for k in range(2):
        row = jnp.dot(pick_ref[k], rows, preferred_element_type=F32)
        mixed = mixed + row * weight_ref[k]
    mixed_ref[...] = mixed
    square = jnp.sum((mixed * mixed).T, axis=0, keepdims=True)
    for t in range(TP):
        square_ref[t] = square


def finish_kernel(mixed_ref, square_ref, gain_ref, out_ref):
    square = jnp.zeros((1, TOK), F32)
    for t in range(TP):
        square = square + square_ref[t]
    column = jnp.broadcast_to(lax.rsqrt(square / D + EPS), (TOK, TOK)).T
    out_ref[...] = (mixed_ref[...] * column * gain_ref[...]).astype(BF16)


def shards(
    tokens, norm_gain, routing, route_weight, gate_weight, up_weight, down_weight, final_gain
):
    swap = [(0, 1), (1, 0)]
    gate_own, up_own = gate_weight[0].T, up_weight[0].T
    outgoing, place, gain_parts = call(
        dispatch_kernel,
        [((EXPERTS, 2, 640), BF16), ((2, TOK), jnp.int32), ((EXTRA, W), BF16)],
        4,
        hbm=3,
        far_out=True,
        scratch_shapes=[
            pltpu.VMEM((2, TOK), jnp.int32),
            pltpu.VMEM((TOK, W), BF16),
            pltpu.VMEM((1, W), F32),
            pltpu.VMEM((EXPERTS, 2, 640), BF16),
            pltpu.SemaphoreType.DMA((4,)),
        ],
    )(routing.T, tokens, norm_gain.reshape(1, W))
    arrived = exchange(outgoing, FIRST)
    gate_other = lax.ppermute(gate_own, "c", swap)
    up_other = lax.ppermute(up_own, "c", swap)
    pick, weight = call(
        prepare_kernel,
        [((2, TOK, ROWS), BF16), ((2, TOK, W), F32)],
        4,
    )(place, route_weight.T)
    spread = call(
        spread_kernel,
        ((TP, FRONT + HID, W), BF16),
        4,
        hbm=1,
        scratch_shapes=[pltpu.SemaphoreType.DMA((TP,))],
    )(
        arrived, gain_parts, down_weight.reshape(TP, HID, W)
    )
    features = across_plane(spread)
    down_other = lax.ppermute(features[:, FRONT:], "c", swap)
    hidden = call(
        hidden_kernel,
        ((2, ROWS, HID), BF16),
        16,
        scratch_shapes=[pltpu.VMEM((ROWS, D), BF16)],
    )(features, gate_own, gate_other, up_own, up_other)
    parts = call(output_kernel, ((TP, ROWS, W), BF16), 8)(
        hidden, features, down_other
    )
    parts = across_plane(parts)
    reduced = call(reduce_kernel, ((EXPERTS, 2, 640), BF16), 4)(parts)
    returned = exchange(reduced, BACK)
    mixed, square = call(
        combine_kernel, [((TOK, W), F32), ((TP, 1, TOK), F32)], 4
    )(returned, pick, weight)
    squares = across_plane(square)
    return call(finish_kernel, ((TOK, W), BF16), 4)(mixed, squares, final_gain.reshape(1, W))


def solution(mesh):
    split = Mesh(mesh.devices.reshape(EXPERTS, 2, TP), ("z", "c", "t"))
    ep = ("z", "c")
    placed = (
        P(ep, "t"),
        P("t"),
        P(ep, None),
        P(ep, None),
        P(ep, None, "t"),
        P(ep, None, "t"),
        P(ep, None, "t"),
        P("t"),
    )
    return jax.shard_map(
        shards, mesh=split, in_specs=placed, out_specs=P(ep, "t"), check_vma=False
    )
```
